1024 devices in a mesh: sp: 256 (over z, y, core), tp: 4 (over x).
Axes of the slice: x: 4, y: 8, z: 16, core: 2. Of those that a mesh axis runs over, the one named last changes fastest.
Arguments:
- tokens: bfloat16 [65536, 2048], P('sp'), may hold values from -28 to 28
- query_weight: bfloat16 [2048, 1536], P(None, 'tp'), may hold values from -0.125 to 0.125
- key_weight: bfloat16 [2048, 1536], P(None, 'tp'), may hold values from -0.125 to 0.125
- value_weight: bfloat16 [2048, 1536], P(None, 'tp'), may hold values from -0.125 to 0.125
- out_weight: bfloat16 [512, 2048], P(None, 'tp'), may hold values from -1 to 1
Outputs:
- mixed: bfloat16 [65536, 2048], P('sp', 'tp')
- total_log: float32 [4, 65536], P('tp', 'sp')
The draws below stay inside these ranges and needn't reach their ends.
All inputs are finite; a program needn't handle non-finite values.
Results may differ from the reference program's by a relative error of at most 0.012.
The reference program's roundings to bfloat16 on the way (of `queries`, `probs` and `merged`) count: a program that leaves them out, or rounds other values in their place, can miss the bound.
Values may be sent and summed in bfloat16 or wider, within the bound.
No kernel may reach another device: no remote copies, remote signals or barrier semaphores. Data moves between devices by JAX's collectives and lax.ppermute only.
A program may use at most 64 MiB of HBM per device.

```python
import jax
import jax.numpy as jnp
from jax import lax

D = 2048
HEADS = 4
HEAD_DIM = 128
NEAR_WINDOW = 128
MIDDLE_WINDOW = 512
MIDDLE_DILATION = 4
FAR_WINDOW = 2048
FAR_DILATION = 16
TOK_DEV = 256
TOKENS = 65536
N_SP = 256


def draw_tokens(key, part):
    first_key, second_key, third_key = jax.random.split(key, 3)
    return jnp.clip(jax.random.normal(first_key, (TOKENS, D), jnp.float32), -6.0, 6.0).astype(jnp.bfloat16)


def block_scale(key, extent, cuts, low, largest):
    loudness = 1.0
    for axis_at, shards_of in cuts:
        steps = jax.random.uniform(jax.random.fold_in(jax.random.fold_in(key, 6), axis_at), (shards_of,), jnp.float32, low / len(cuts), largest / len(cuts))
        loudness = loudness * jnp.repeat(jnp.exp(steps), extent[axis_at] // shards_of).reshape((-1,) + (1,) * (len(extent) - 1 - axis_at))
    return loudness


def gaussian(own_key, dims, deviation, limit, cuts=(), kind=jnp.bfloat16):
    level = block_scale(own_key, dims, cuts, -0.22, 0.18) if cuts else 1.0
    array = jax.random.normal(own_key, dims, jnp.float32) * deviation * level
    return jnp.minimum(jnp.maximum(array, -limit), limit).astype(kind)


def setup_inputs(seed: int = 0) -> dict:
    splits = jax.random.split(jax.random.key(seed), 6)
    tokens = draw_tokens(jax.random.fold_in(splits[5], 71), 0)
    query_weight = gaussian(splits[1], (D, HEADS * 3 * HEAD_DIM), D ** -0.5, 0.125, ((1, 4),))
    key_weight = gaussian(splits[2], (D, HEADS * 3 * HEAD_DIM), D ** -0.5, 0.125, ((1, 4),))
    value_weight = gaussian(splits[3], (D, HEADS * 3 * HEAD_DIM), D ** -0.5, 0.125, ((1, 4),))
    out_weight = gaussian(splits[4], (HEADS * HEAD_DIM, D), (HEADS * HEAD_DIM // 16) ** -0.5, 1.0, ((1, 4),))
    return dict(tokens=tokens, query_weight=query_weight, key_weight=key_weight, value_weight=value_weight, out_weight=out_weight)


def window_table():
    return ((NEAR_WINDOW, 1), (MIDDLE_WINDOW, MIDDLE_DILATION), (FAR_WINDOW, FAR_DILATION))


def attend_group(group_queries, buffer, window, dilation, first_key, slopes_here):
    row_count = group_queries.shape[0]
    head_count = group_queries.shape[1]
    head_size = group_queries.shape[2]
    query_split = group_queries.reshape(row_count // dilation, dilation, head_count, head_size)
    key_split = buffer[0].reshape(-1, dilation, head_count, head_size)
    value_split = buffer[1].reshape(-1, dilation, head_count, head_size)
    scores = jnp.einsum("mrhe,nrhe->rhmn", query_split.astype(jnp.float32), key_split.astype(jnp.float32)) * head_size ** -0.5
    grid_shape = (row_count // dilation, key_split.shape[0])
    query_slot = lax.broadcasted_iota(jnp.int32, grid_shape, 0)
    key_slot = lax.broadcasted_iota(jnp.int32, grid_shape, 1)
    spacing = query_slot + window // dilation - key_slot
    residue = lax.broadcasted_iota(jnp.int32, (dilation, 1, 1), 0)
    key_place = first_key + residue + dilation * key_slot[None]
    valid = (spacing[None] >= 0) & (spacing[None] <= window // dilation) & (key_place >= 0)
    scores = scores - slopes_here[None, :, None, None] * (dilation * spacing).astype(scores.dtype)[None, None]
    masked = jnp.where(valid[:, None], scores, -jnp.inf)
    highest = jnp.max(masked, axis=-1, keepdims=True)
    log_sum = highest + jnp.log(jnp.sum(jnp.exp(masked - highest), axis=-1, keepdims=True))
    probs = jnp.exp(masked - log_sum).astype(jnp.bfloat16)
    attended = jnp.einsum("rhmn,nrhe->mrhe", probs.astype(jnp.float32), value_split.astype(jnp.float32))
    attended = attended.reshape(row_count, head_count, head_size)
    log_rows = jnp.transpose(log_sum[..., 0], (1, 2, 0)).reshape(head_count, row_count)
    return attended, log_rows


def reference(tokens, query_weight, key_weight, value_weight, out_weight):
    def project(weight_matrix):
        product = jnp.dot(tokens, weight_matrix, preferred_element_type=jnp.float32)
        return product.astype(jnp.bfloat16).reshape(TOKENS, HEADS, 3, HEAD_DIM)

    queries = project(query_weight)
    keys_all = project(key_weight)
    values_all = project(value_weight)
    stacked = jnp.stack((keys_all, values_all))
    padding = jnp.zeros((2, FAR_WINDOW, HEADS, 3, HEAD_DIM), stacked.dtype)
    padded = jnp.concatenate((padding, stacked), axis=1)
    head_ids = jnp.arange(HEADS).astype(jnp.float32)

    def block_step(block_index):
        first_row = block_index * TOK_DEV
        query_block = lax.dynamic_slice_in_dim(queries, first_row, TOK_DEV, 0)
        outputs = []
        logs = []
        for group_index, (window, dilation) in enumerate(window_table()):
            begin = (first_row + FAR_WINDOW - window).astype(jnp.int32)
            buffer = lax.dynamic_slice_in_dim(padded, begin, window + TOK_DEV, 1)[:, :, :, group_index]
            slopes_here = 2.0 ** (3.0 - 8.0 * (head_ids + 1.0) / HEADS) / window
            attended, log_rows = attend_group(query_block[:, :, group_index], buffer, window, dilation, first_row - window, slopes_here)
            outputs.append(attended)
            logs.append(log_rows)
        stacked_logs = jnp.stack(logs)
        highest = jnp.max(stacked_logs, axis=0)
        total_block = highest + jnp.log(jnp.sum(jnp.exp(stacked_logs - highest), axis=0))
        mixing = jnp.exp(stacked_logs - total_block)
        merged_block = outputs[0] * jnp.transpose(mixing[0])[:, :, None]
        merged_block = merged_block + outputs[1] * jnp.transpose(mixing[1])[:, :, None]
        merged_block = merged_block + outputs[2] * jnp.transpose(mixing[2])[:, :, None]
        return merged_block.astype(jnp.bfloat16), total_block

    merged_blocks, totals = lax.map(block_step, jnp.arange(N_SP, dtype=jnp.int32))
    merged = merged_blocks.reshape(TOKENS, HEADS * HEAD_DIM)
    mixed = jnp.dot(merged, out_weight, preferred_element_type=jnp.float32).astype(jnp.bfloat16)
    total_log = jnp.transpose(totals, (1, 0, 2)).reshape(HEADS, TOKENS)
    return mixed, total_log
```

```python
import jax
import jax.numpy as jnp
from jax import lax
from jax.experimental import pallas as pl
from jax.experimental.pallas import tpu as pltpu
from jax.sharding import Mesh
from jax.sharding import PartitionSpec as P

HEAD_DIM = 128
TOK = 256
PLANE = 16
RUN = TOK // PLANE
BAND = 128
MIDDLE_DILATION = 4
SCALE = HEAD_DIM**-0.5
K_STEPS = 4
F32 = jnp.float32
BF16 = jnp.bfloat16
VMEM = pltpu.VMEM
WHOLE = pl.BlockSpec(memory_space=pltpu.VMEM)


def iota(shape, dim):
    return lax.broadcasted_iota(jnp.int32, shape, dim)


def residue_order():
    row, col = iota((TOK, TOK), 0), iota((TOK, TOK), 1)
    return jnp.where(col == (row % RUN) * PLANE + row // RUN, 1.0, 0.0).astype(BF16)


def head_slope():
    head = lax.axis_index("tp")
    return jnp.where(head == 0, 2.0, jnp.where(head == 1, 0.5, jnp.where(head == 2, 0.125, 0.03125)))


def times_transposed(a, b):
    return lax.dot_general(a, b, (((1,), (1,)), ((), ())), preferred_element_type=F32)


def soft(scores, valid, values):
    scores = jnp.where(valid, scores, -jnp.inf)
    highest = jnp.max(scores, axis=1, keepdims=True)
    weights = jnp.exp(scores - highest)
    total = jnp.sum(weights, axis=1, keepdims=True)
    probs = (weights * (1.0 / total)).astype(BF16)
    return jnp.dot(probs, values, preferred_element_type=F32), highest + jnp.log(total)


def banded(queries, keys, values, slope, has_prior):
    shape = (TOK, TOK + BAND)
    spacing = iota(shape, 0) + BAND - iota(shape, 1)
    first = jnp.where(has_prior, 0, BAND)
    valid = (spacing >= 0) & (spacing <= BAND) & (iota(shape, 1) >= first)
    scores = times_transposed(queries, keys) * SCALE - slope * spacing.astype(F32)
    return soft(scores, valid, values)


def project_body(tok, wq, wk, wv, far, queries, near, sent_one, sent_two, acc):
    step = pl.program_id(0)

    @pl.when(step == 0)
    def _():
        acc[...] = jnp.zeros_like(acc)

    x = tok[...]
    for j, w in enumerate((wq, wk, wv)):
        acc[j] += jnp.dot(x, w[...], preferred_element_type=F32)

    @pl.when(step == pl.num_programs(0) - 1)
    def _():
        q, k, v = acc[0].astype(BF16), acc[1].astype(BF16), acc[2].astype(BF16)
        d = HEAD_DIM
        order = residue_order()
        for j, part in enumerate((q, k, v)):
            sorted_rows = jnp.dot(order, part[:, 2 * d :], preferred_element_type=F32).astype(BF16)
            far[:, j * RUN : (j + 1) * RUN] = sorted_rows.reshape(PLANE, RUN, d)
        queries[0] = q[:, :d]
        queries[1] = q[:, d : 2 * d]
        near[0] = k[:BAND, :d]
        near[1] = v[:BAND, :d]
        sent_one[:BAND] = k[BAND:, :d]
        sent_one[BAND : 2 * BAND] = v[BAND:, :d]
        for j, part in enumerate((k, v)):
            rows = part[:, d : 2 * d]
            sent_one[2 * BAND + j * TOK : 2 * BAND + (j + 1) * TOK] = rows
            sent_two[j * TOK : (j + 1) * TOK] = rows


def project(tokens, wq, wk, wv):
    width, cols = wq.shape
    chunk = width // K_STEPS
    d = HEAD_DIM
    weight = pl.BlockSpec((chunk, cols), lambda i: (i, 0))
    return pl.pallas_call(
        project_body,
        grid=(K_STEPS,),
        in_specs=[pl.BlockSpec((TOK, chunk), lambda i: (0, i)), weight, weight, weight],
        out_specs=[WHOLE] * 5,
        out_shape=[
            VMEM((PLANE, 3 * RUN, d), BF16),
            VMEM((2, TOK, d), BF16),
            VMEM((2, BAND, d), BF16),
            VMEM((2 * BAND + 2 * TOK, d), BF16),
            VMEM((2 * TOK, d), BF16),
        ],
        scratch_shapes=[pltpu.VMEM((3, TOK, cols), F32)],
        name="project",
    )(tokens, wq, wk, wv)


def near_middle_body(queries, near, own, one, two, attended, log):
    slope = head_slope()
    place = lax.axis_index("z") * PLANE + lax.axis_index("yc")
    b = BAND
    keys = jnp.concatenate((one[:b], near[0], own[:b]), axis=0)
    values = jnp.concatenate((one[b : 2 * b], near[1], own[b : 2 * b]), axis=0)
    first, first_log = banded(queries[0], keys, values, slope / b, place > 0)

    k_at, v_at = slice(2 * b, 2 * b + TOK), slice(2 * b + TOK, 2 * b + 2 * TOK)
    keys = jnp.concatenate((two[:TOK], one[k_at], own[k_at]), axis=0)
    values = jnp.concatenate((two[TOK:], one[v_at], own[v_at]), axis=0)
    shape = (TOK, 3 * TOK)
    window = MIDDLE_DILATION * BAND
    spacing = iota(shape, 0) + window - iota(shape, 1)
    begin = jnp.maximum(window - place * TOK, 0)
    valid = (spacing >= 0) & (spacing <= window) & (spacing % MIDDLE_DILATION == 0)
    valid = valid & (iota(shape, 1) >= begin)
    scores = times_transposed(queries[1], keys) * SCALE - (slope / window) * spacing.astype(F32)
    second, second_log = soft(scores, valid, values)

    highest = jnp.maximum(first_log, second_log)
    first_share, second_share = jnp.exp(first_log - highest), jnp.exp(second_log - highest)
    total = first_share + second_share
    inverse = 1.0 / total
    attended[...] = (first_share * inverse) * first + (second_share * inverse) * second
    log[...] = jnp.broadcast_to(highest + jnp.log(total), log.shape)


def near_middle(queries, near, own, one, two):
    shape = (TOK, HEAD_DIM)
    return pl.pallas_call(
        near_middle_body,
        in_specs=[WHOLE] * 5,
        out_specs=[WHOLE] * 2,
        out_shape=[VMEM(shape, F32), VMEM(shape, F32)],
        name="near_middle",
    )(queries, near, own, one, two)


def far_body(mine, halo, out):
    d, r = HEAD_DIM, RUN
    slope = head_slope() / BAND
    queries = mine[:, :r].reshape(TOK, d)
    keys = jnp.concatenate((halo[:, :r].reshape(BAND, d), mine[:, r : 2 * r].reshape(TOK, d)), axis=0)
    values = jnp.concatenate((halo[:, r:].reshape(BAND, d), mine[:, 2 * r :].reshape(TOK, d)), axis=0)
    attended, log = banded(queries, keys, values, slope, lax.axis_index("z") > 0)
    out[:, :r] = attended.astype(BF16).reshape(PLANE, r, d)
    lanes = iota((TOK, d), 1)
    slots = iota((TOK, d), 0) % r
    rows = jnp.sum(jnp.where(lanes == slots, log, 0.0).reshape(PLANE, r, d), axis=1)
    high = rows.astype(BF16).astype(F32)
    middle = (rows - high).astype(BF16).astype(F32)
    low = rows - high - middle
    at = iota((PLANE, 8, d), 1)
    parts = jnp.where(at == 0, high[:, None], jnp.where(at == 1, middle[:, None], low[:, None]))
    out[:, r:] = jnp.where(at < 3, parts, 0.0).astype(BF16)


def far_attention(mine, halo):
    return pl.pallas_call(
        far_body,
        in_specs=[WHOLE] * 2,
        out_specs=WHOLE,
        out_shape=VMEM((PLANE, RUN + 8, HEAD_DIM), BF16),
        name="far",
    )(mine, halo)


def merge_body(attended, log, far, merged, total_log):
    d, r = HEAD_DIM, RUN
    rows = far[:, :r].reshape(TOK, d)
    far_rows = jnp.dot(residue_order(), rows, preferred_element_type=F32)
    logs = jnp.sum(far[:, r:].astype(F32), axis=1)
    spread = jnp.broadcast_to(logs[None], (RUN, PLANE, d)).reshape(TOK, d)
    tokens, lanes = iota((TOK, d), 0), iota((TOK, d), 1)
    far_log = jnp.sum(jnp.where(lanes == tokens // PLANE, spread, 0.0), axis=1, keepdims=True)
    other_log = log[:, :1]
    highest = jnp.maximum(other_log, far_log)
    total = highest + jnp.log(jnp.exp(other_log - highest) + jnp.exp(far_log - highest))
    both = jnp.exp(other_log - total) * attended[...] + jnp.exp(far_log - total) * far_rows
    both = both.astype(BF16)
    for j in range(merged.shape[0]):
        merged[j] = both
    for j in range(TOK // d):
        part = jnp.where(lanes == tokens - j * d, total, 0.0)
        total_log[:, j * d : (j + 1) * d] = jnp.sum(part, axis=0, keepdims=True)


def merge(attended, log, far, copies):
    return pl.pallas_call(
        merge_body,
        in_specs=[WHOLE] * 3,
        out_specs=[WHOLE] * 2,
        out_shape=[VMEM((copies, TOK, HEAD_DIM), BF16), jax.ShapeDtypeStruct((1, TOK), F32)],
        name="merge",
    )(attended, log, far)


def mix_body(heads, weight, out):
    rows = jnp.concatenate([heads[j] for j in range(heads.shape[0])], axis=1)
    out[...] = jnp.dot(rows, weight[...], preferred_element_type=F32).astype(BF16)


def mix(heads, weight):
    return pl.pallas_call(
        mix_body,
        in_specs=[WHOLE] * 2,
        out_specs=WHOLE,
        out_shape=jax.ShapeDtypeStruct((TOK, weight.shape[1]), BF16),
        name="mix",
    )(heads, weight)


def swap(blocks, axis):
    return lax.all_to_all(blocks, axis, split_axis=0, concat_axis=0, tiled=True)


def behind(block, axes, distance):
    count = lax.axis_size(axes)
    return lax.ppermute(block, axes, [(i - distance, i) for i in range(distance, count)])


def local(tokens, query_weight, key_weight, value_weight, out_weight):
    sp = ("z", "yc")
    far, queries, near, sent_one, sent_two = project(tokens, query_weight, key_weight, value_weight)
    mine = swap(far, "yc")
    one, two = behind(sent_one, sp, 1), behind(sent_two, sp, 2)
    halo = behind(mine[PLANE // 2 :, RUN:], "z", 1)
    attended, log = near_middle(queries, near, sent_one, one, two)
    far_out = swap(far_attention(mine, halo), "yc")
    merged, total_log = merge(attended, log, far_out, lax.axis_size("tp"))
    return mix(swap(merged, "tp"), out_weight), total_log


def solution(mesh):
    devices = mesh.devices
    planes = Mesh(devices.reshape(devices.shape[0] // PLANE, PLANE, devices.shape[1]), ("z", "yc", "tp"))
    sp = ("z", "yc")
    return jax.shard_map(
        local,
        mesh=planes,
        in_specs=(P(sp, None), P(None, "tp"), P(None, "tp"), P(None, "tp"), P(None, "tp")),
        out_specs=(P(sp, "tp"), P("tp", sp)),
        check_vma=False,
    )
```

```python
import jax
import jax.numpy as jnp
from jax import lax
from jax.experimental import pallas as pl
from jax.experimental.pallas import tpu as pltpu
from jax.sharding import Mesh
from jax.sharding import PartitionSpec as P

HEAD_DIM = 128
TOK = 256
PLANE = 16
RUN = TOK // PLANE
BAND = 128
MIDDLE_DILATION = 4
SCALE = HEAD_DIM**-0.5
F32 = jnp.float32
BF16 = jnp.bfloat16
VMEM = pltpu.VMEM
WHOLE = pl.BlockSpec(memory_space=pltpu.VMEM)


def held(*arrays):
    return [pltpu.with_memory_space_constraint(a, pltpu.VMEM) for a in arrays]


def iota(shape, dim):
    return lax.broadcasted_iota(jnp.int32, shape, dim)


def residue_order():
    row, col = iota((TOK, TOK), 0), iota((TOK, TOK), 1)
    return jnp.where(col == (row % RUN) * PLANE + row // RUN, 1.0, 0.0).astype(BF16)


def head_slope():
    head = lax.axis_index("tp")
    return jnp.where(head == 0, 2.0, jnp.where(head == 1, 0.5, jnp.where(head == 2, 0.125, 0.03125)))


def times_transposed(a, b):
    return lax.dot_general(a, b, (((1,), (1,)), ((), ())), preferred_element_type=F32)


def soft(scores, valid, values):
    scores = jnp.where(valid, scores, -jnp.inf)
    highest = jnp.max(scores, axis=1, keepdims=True)
    weights = jnp.exp(scores - highest)
    total = jnp.sum(weights, axis=1, keepdims=True)
    probs = (weights * (1.0 / total)).astype(BF16)
    return jnp.dot(probs, values, preferred_element_type=F32), highest + jnp.log(total)


def banded(queries, keys, values, slope, has_prior):
    shape = (TOK, TOK + BAND)
    spacing = iota(shape, 0) + BAND - iota(shape, 1)
    first = jnp.where(has_prior, 0, BAND)
    valid = (spacing >= 0) & (spacing <= BAND) & (iota(shape, 1) >= first)
    scores = times_transposed(queries, keys) * SCALE - slope * spacing.astype(F32)
    return soft(scores, valid, values)


def project_body(tok_hbm, wq_hbm, wk_hbm, wv_hbm, far, queries, near, sent_one, sent_two, tok, wq, wk, wv, sems):
    pairs = ((tok_hbm, tok), (wk_hbm, wk), (wv_hbm, wv), (wq_hbm, wq))
    copies = []
    for j, (source, target) in enumerate(pairs):
        half = source.shape[0] // 2
        parts = [
            pltpu.make_async_copy(source.at[pl.ds(i * half, half)], target.at[pl.ds(i * half, half)], sems.at[j, i])
            for i in range(2)
        ]
        for part in parts:
            part.start()
        copies.append(parts)

    def arrive(j):
        for part in copies[j]:
            part.wait()

    def times(weight):
        return jnp.dot(tok[...], weight[...], preferred_element_type=F32).astype(BF16)

    d = HEAD_DIM
    order = residue_order()

    def put_far(j, rows):
        rows = jnp.dot(order, rows[:, 2 * d :], preferred_element_type=F32).astype(BF16)
        far[:, j * RUN : (j + 1) * RUN] = rows.reshape(PLANE, RUN, d)

    def put_sent(j, rows):
        near[j] = rows[:BAND, :d]
        sent_one[j * BAND : (j + 1) * BAND] = rows[BAND:, :d]
        sent_one[2 * BAND + j * TOK : 2 * BAND + (j + 1) * TOK] = rows[:, d : 2 * d]
        sent_two[j * TOK : (j + 1) * TOK] = rows[:, d : 2 * d]

    arrive(0)
    arrive(1)
    rows = times(wk)
    put_far(1, rows)
    put_sent(0, rows)
    arrive(2)
    rows = times(wv)
    put_far(2, rows)
    put_sent(1, rows)
    arrive(3)
    rows = times(wq)
    put_far(0, rows)
    queries[0] = rows[:, :d]
    queries[1] = rows[:, d : 2 * d]


def project(tokens, wq, wk, wv):
    d = HEAD_DIM
    in_hbm = pl.BlockSpec(memory_space=pl.ANY)
    return pl.pallas_call(
        project_body,
        in_specs=[in_hbm] * 4,
        out_specs=[WHOLE] * 5,
        out_shape=[
            VMEM((PLANE, 3 * RUN, d), BF16),
            VMEM((2, TOK, d), BF16),
            VMEM((2, BAND, d), BF16),
            VMEM((2 * BAND + 2 * TOK, d), BF16),
            VMEM((2 * TOK, d), BF16),
        ],
        scratch_shapes=[pltpu.VMEM(a.shape, a.dtype) for a in (tokens, wq, wk, wv)] + [pltpu.SemaphoreType.DMA((4, 2))],
        name="project",
    )(*[pltpu.with_memory_space_constraint(a, pltpu.HBM) for a in (tokens, wq, wk, wv)])


def near_middle_body(queries, near, own, one, two, attended, log):
    slope = head_slope()
    place = lax.axis_index("z") * PLANE + lax.axis_index("yc")
    b = BAND
    keys = jnp.concatenate((one[:b], near[0], own[:b]), axis=0)
    values = jnp.concatenate((one[b : 2 * b], near[1], own[b : 2 * b]), axis=0)
    first, first_log = banded(queries[0], keys, values, slope / b, place > 0)

    k_at, v_at = slice(2 * b, 2 * b + TOK), slice(2 * b + TOK, 2 * b + 2 * TOK)
    keys = jnp.concatenate((two[:TOK], one[k_at], own[k_at]), axis=0)
    values = jnp.concatenate((two[TOK:], one[v_at], own[v_at]), axis=0)
    shape = (TOK, 3 * TOK)
    window = MIDDLE_DILATION * BAND
    spacing = iota(shape, 0) + window - iota(shape, 1)
    begin = jnp.maximum(window - place * TOK, 0)
    valid = (spacing >= 0) & (spacing <= window) & (spacing % MIDDLE_DILATION == 0)
    valid = valid & (iota(shape, 1) >= begin)
    scores = times_transposed(queries[1], keys) * SCALE - (slope / window) * spacing.astype(F32)
    second, second_log = soft(scores, valid, values)

    highest = jnp.maximum(first_log, second_log)
    first_share, second_share = jnp.exp(first_log - highest), jnp.exp(second_log - highest)
    total = first_share + second_share
    inverse = 1.0 / total
    attended[...] = (first_share * inverse) * first + (second_share * inverse) * second
    log[...] = jnp.broadcast_to(highest + jnp.log(total), log.shape)


def near_middle(queries, near, own, one, two):
    shape = (TOK, HEAD_DIM)
    return pl.pallas_call(
        near_middle_body,
        in_specs=[WHOLE] * 5,
        out_specs=[WHOLE] * 2,
        out_shape=[VMEM(shape, F32), VMEM(shape, F32)],
        name="near_middle",
    )(*held(queries, near, own, one, two))


def far_body(mine, halo, out):
    d, r = HEAD_DIM, RUN
    slope = head_slope() / BAND
    queries = mine[:, :r].reshape(TOK, d)
    keys = jnp.concatenate((halo[:, :r].reshape(BAND, d), mine[:, r : 2 * r].reshape(TOK, d)), axis=0)
    values = jnp.concatenate((halo[:, r:].reshape(BAND, d), mine[:, 2 * r :].reshape(TOK, d)), axis=0)
    attended, log = banded(queries, keys, values, slope, lax.axis_index("z") > 0)
    out[:, :r] = attended.astype(BF16).reshape(PLANE, r, d)
    lanes = iota((TOK, d), 1)
    slots = iota((TOK, d), 0) % r
    rows = jnp.sum(jnp.where(lanes == slots, log, 0.0).reshape(PLANE, r, d), axis=1)
    high = rows.astype(BF16).astype(F32)
    middle = (rows - high).astype(BF16).astype(F32)
    low = rows - high - middle
    at = iota((PLANE, 8, d), 1)
    parts = jnp.where(at == 0, high[:, None], jnp.where(at == 1, middle[:, None], low[:, None]))
    out[:, r:] = jnp.where(at < 3, parts, 0.0).astype(BF16)


def far_attention(mine, halo):
    return pl.pallas_call(
        far_body,
        in_specs=[WHOLE] * 2,
        out_specs=WHOLE,
        out_shape=VMEM((PLANE, RUN + 8, HEAD_DIM), BF16),
        name="far",
    )(*held(mine, halo))


def merge_body(attended, log, far, merged, total_log):
    d, r = HEAD_DIM, RUN
    rows = far[:, :r].reshape(TOK, d)
    far_rows = jnp.dot(residue_order(), rows, preferred_element_type=F32)
    logs = jnp.sum(far[:, r:].astype(F32), axis=1)
    spread = jnp.broadcast_to(logs[None], (RUN, PLANE, d)).reshape(TOK, d)
    tokens, lanes = iota((TOK, d), 0), iota((TOK, d), 1)
    far_log = jnp.sum(jnp.where(lanes == tokens // PLANE, spread, 0.0), axis=1, keepdims=True)
    other_log = log[:, :1]
    highest = jnp.maximum(other_log, far_log)
    total = highest + jnp.log(jnp.exp(other_log - highest) + jnp.exp(far_log - highest))
    both = jnp.exp(other_log - total) * attended[...] + jnp.exp(far_log - total) * far_rows
    both = both.astype(BF16)
    for j in range(merged.shape[0]):
        merged[j] = both
    for j in range(TOK // d):
        part = jnp.where(lanes == tokens - j * d, total, 0.0)
        total_log[:, j * d : (j + 1) * d] = jnp.sum(part, axis=0, keepdims=True)


def merge(attended, log, far, copies):
    return pl.pallas_call(
        merge_body,
        in_specs=[WHOLE] * 3,
        out_specs=[WHOLE] * 2,
        out_shape=[VMEM((copies, TOK, HEAD_DIM), BF16), VMEM((1, TOK), F32)],
        name="merge",
    )(*held(attended, log, far))


def mix_body(heads, weight, out):
    rows = jnp.concatenate([heads[j] for j in range(heads.shape[0])], axis=1)
    out[...] = jnp.dot(rows, weight[...], preferred_element_type=F32).astype(BF16)


def mix(heads, weight):
    return pl.pallas_call(
        mix_body,
        in_specs=[WHOLE] * 2,
        out_specs=WHOLE,
        out_shape=jax.ShapeDtypeStruct((TOK, weight.shape[1]), BF16),
        name="mix",
    )(*held(heads, weight))


def swap(blocks, axis):
    return lax.all_to_all(blocks, axis, split_axis=0, concat_axis=0, tiled=True)


def behind(block, axes, distance):
    count = lax.axis_size(axes)
    return lax.ppermute(block, axes, [(i - distance, i) for i in range(distance, count)])


def local(tokens, query_weight, key_weight, value_weight, out_weight):
    sp = ("z", "yc")
    far, queries, near, sent_one, sent_two = project(tokens, query_weight, key_weight, value_weight)
    mine = swap(far, "yc")
    one, two = behind(sent_one, sp, 1), behind(sent_two, sp, 2)
    halo = behind(mine[PLANE // 2 :, RUN:], "z", 1)
    attended, log = near_middle(queries, near, sent_one, one, two)
    far_out = swap(far_attention(mine, halo), "yc")
    merged, total_log = merge(attended, log, far_out, lax.axis_size("tp"))
    return mix(swap(merged, "tp"), out_weight), total_log


def solution(mesh):
    devices = mesh.devices
    planes = Mesh(devices.reshape(devices.shape[0] // PLANE, PLANE, devices.shape[1]), ("z", "yc", "tp"))
    sp = ("z", "yc")
    return jax.shard_map(
        local,
        mesh=planes,
        in_specs=(P(sp, None), P(None, "tp"), P(None, "tp"), P(None, "tp"), P(None, "tp")),
        out_specs=(P(sp, "tp"), P("tp", sp)),
        check_vma=False,
    )
```

```python
import jax
import jax.numpy as jnp
from jax import lax
from jax.experimental import pallas as pl
from jax.experimental.pallas import tpu as pltpu
from jax.sharding import Mesh
from jax.sharding import PartitionSpec as P

HEAD_DIM = 128
TOK = 256
PLANE = 16
BAND = 128
MIDDLE_DILATION = 4
FAR_DILATION = 16
REACH = 8
SCALE = HEAD_DIM**-0.5
F32 = jnp.float32
BF16 = jnp.bfloat16
VMEM = pltpu.VMEM
WHOLE = pl.BlockSpec(memory_space=pltpu.VMEM)


def held(*arrays):
    return [pltpu.with_memory_space_constraint(a, pltpu.VMEM) for a in arrays]


def iota(shape, dim):
    return lax.broadcasted_iota(jnp.int32, shape, dim)


def head_slope():
    head = lax.axis_index("tp")
    return jnp.where(head == 0, 2.0, jnp.where(head == 1, 0.5, jnp.where(head == 2, 0.125, 0.03125)))


def times_transposed(a, b):
    return lax.dot_general(a, b, (((1,), (1,)), ((), ())), preferred_element_type=F32)


def soft(scores, valid, values):
    scores = jnp.where(valid, scores, -jnp.inf)
    highest = jnp.max(scores, axis=1, keepdims=True)
    weights = jnp.exp(scores - highest)
    total = jnp.sum(weights, axis=1, keepdims=True)
    probs = (weights * (1.0 / total)).astype(BF16)
    return jnp.dot(probs, values, preferred_element_type=F32), highest + jnp.log(total)


def banded(queries, keys, values, slope, has_prior):
    shape = (TOK, TOK + BAND)
    spacing = iota(shape, 0) + BAND - iota(shape, 1)
    first = jnp.where(has_prior, 0, BAND)
    valid = (spacing >= 0) & (spacing <= BAND) & (iota(shape, 1) >= first)
    scores = times_transposed(queries, keys) * SCALE - slope * spacing.astype(F32)
    return soft(scores, valid, values)


def project_body(tok_hbm, wq_hbm, wk_hbm, wv_hbm, queries, near, far, pack, tok, wq, wk, wv, sems):
    pairs = ((tok_hbm, tok), (wk_hbm, wk), (wv_hbm, wv), (wq_hbm, wq))
    copies = []
    for j, (source, target) in enumerate(pairs):
        half = source.shape[0] // 2
        parts = [
            pltpu.make_async_copy(source.at[pl.ds(i * half, half)], target.at[pl.ds(i * half, half)], sems.at[j, i])
            for i in range(2)
        ]
        for part in parts:
            part.start()
        copies.append(parts)

    def arrive(j):
        for part in copies[j]:
            part.wait()

    d = HEAD_DIM
    arrive(0)
    for j, weight in enumerate((wk, wv)):
        arrive(j + 1)
        rows = jnp.dot(tok[...], weight[...], preferred_element_type=F32).astype(BF16)
        far[j * TOK : (j + 1) * TOK] = rows[:, 2 * d :]
        pack[j * TOK : (j + 1) * TOK] = rows[:, 2 * d :]
        pack[(2 + j) * TOK : (3 + j) * TOK] = rows[:, d : 2 * d]
        near[j] = rows[:BAND, :d]
        pack[4 * TOK + j * BAND : 4 * TOK + (j + 1) * BAND] = rows[BAND:, :d]
    arrive(3)
    rows = jnp.dot(tok[...], wq[...], preferred_element_type=F32).astype(BF16)
    for j in range(3):
        queries[j] = rows[:, j * d : (j + 1) * d]


def project(tokens, wq, wk, wv):
    d = HEAD_DIM
    return pl.pallas_call(
        project_body,
        in_specs=[pl.BlockSpec(memory_space=pl.ANY)] * 4,
        out_specs=[WHOLE] * 4,
        out_shape=[
            VMEM((3, TOK, d), BF16),
            VMEM((2, BAND, d), BF16),
            VMEM((2 * TOK, d), BF16),
            VMEM((4 * TOK + 2 * BAND, d), BF16),
        ],
        scratch_shapes=[pltpu.VMEM(a.shape, a.dtype) for a in (tokens, wq, wk, wv)] + [pltpu.SemaphoreType.DMA((4, 2))],
        name="project",
    )(*[pltpu.with_memory_space_constraint(a, pltpu.HBM) for a in (tokens, wq, wk, wv)])


class Far:
    def __init__(self, queries, slope, place):
        self.queries, self.slope, self.place = queries, slope / (FAR_DILATION * BAND), place
        self.apart = iota((TOK, TOK), 0) - iota((TOK, TOK), 1)
        self.bias = jnp.where(self.apart % FAR_DILATION == 0, self.slope * self.apart.astype(F32), jnp.inf)

    def scores(self, places, keys):
        ahead = jnp.where(self.place >= places, self.slope * (TOK * places), jnp.inf)
        part = times_transposed(self.queries, keys) * SCALE - self.bias - ahead
        if places == 0:
            part = jnp.where(self.apart >= 0, part, -jnp.inf)
        if places == REACH:
            part = jnp.where(self.apart <= 0, part, -jnp.inf)
        return part

    def gather(self, blocks, highest=None):
        scores = [self.scores(places, ref[at : at + TOK]) for places, ref, at in blocks]
        top = scores[0]
        for part in scores[1:]:
            top = jnp.maximum(top, part)
        top = jnp.max(top, axis=1, keepdims=True)
        highest = top if highest is None else jnp.maximum(highest, top)
        total, rows = None, None
        for part, (_, ref, at) in zip(scores, blocks):
            weight = jnp.exp(part - highest)
            piece = jnp.dot(weight.astype(BF16), ref[at + TOK : at + 2 * TOK], preferred_element_type=F32)
            total = weight if total is None else total + weight
            rows = piece if rows is None else rows + piece
        return highest, jnp.sum(total, axis=1, keepdims=True), rows


def place_here():
    return lax.axis_index("z") * PLANE + lax.axis_index("yc")


def first_body(queries, near, own, one, two, four, attended, far_rows, stats):
    slope = head_slope()
    place = place_here()
    b, at = BAND, 4 * TOK
    keys = jnp.concatenate((one[at : at + b], near[0], own[at : at + b]), axis=0)
    values = jnp.concatenate((one[at + b : at + 2 * b], near[1], own[at + b : at + 2 * b]), axis=0)
    first, first_log = banded(queries[0], keys, values, slope / b, place > 0)

    k_at, v_at = slice(2 * TOK, 3 * TOK), slice(3 * TOK, 4 * TOK)
    keys = jnp.concatenate((two[k_at], one[k_at], own[k_at]), axis=0)
    values = jnp.concatenate((two[v_at], one[v_at], own[v_at]), axis=0)
    shape = (TOK, 3 * TOK)
    window = MIDDLE_DILATION * BAND
    spacing = iota(shape, 0) + window - iota(shape, 1)
    begin = jnp.maximum(window - place * TOK, 0)
    valid = (spacing >= 0) & (spacing <= window) & (spacing % MIDDLE_DILATION == 0)
    valid = valid & (iota(shape, 1) >= begin)
    scores = times_transposed(queries[1], keys) * SCALE - (slope / window) * spacing.astype(F32)
    second, second_log = soft(scores, valid, values)

    highest = jnp.maximum(first_log, second_log)
    first_share, second_share = jnp.exp(first_log - highest), jnp.exp(second_log - highest)
    total = first_share + second_share
    inverse = 1.0 / total
    attended[...] = (first_share * inverse) * first + (second_share * inverse) * second
    log = highest + jnp.log(total)

    blocks = ((0, own, 0), (1, one, 0), (2, two, 0), (3, one, 4 * TOK + 2 * BAND), (4, four, 0))
    highest, total, rows = Far(queries[2], slope, place).gather(blocks)
    far_rows[...] = rows
    lanes = iota(stats.shape, 1)
    stats[...] = jnp.where(lanes == 0, log, jnp.where(lanes == 1, highest, total))


def first(*arrays):
    shape = (TOK, HEAD_DIM)
    return pl.pallas_call(
        first_body,
        in_specs=[WHOLE] * len(arrays),
        out_specs=[WHOLE] * 3,
        out_shape=[VMEM(shape, F32)] * 3,
        name="first",
    )(*held(*arrays))


def finish_body(queries, odd, six, eight, attended, far_rows, stats, mix_hbm, merged, total_log, mix_weight, sem):
    d = HEAD_DIM
    fetch = pltpu.make_async_copy(mix_hbm, mix_weight, sem)
    fetch.start()
    blocks = ((5, odd, 0), (6, six, 0), (7, odd, 2 * TOK), (8, eight, 0))
    other_log, before, sum_before = stats[:, 0:1], stats[:, 1:2], stats[:, 2:3]
    highest, total, rows = Far(queries[2], head_slope(), place_here()).gather(blocks, before)
    kept = jnp.exp(before - highest)
    total = total + kept * sum_before
    rows = (rows + kept * far_rows[...]) * (1.0 / total)
    far_log = highest + jnp.log(total)

    highest = jnp.maximum(other_log, far_log)
    total = highest + jnp.log(jnp.exp(other_log - highest) + jnp.exp(far_log - highest))
    both = jnp.exp(other_log - total) * attended[...] + jnp.exp(far_log - total) * rows
    both = both.astype(BF16)
    for j in range(merged.shape[0]):
        merged[j] = both
    tokens, lanes = iota((TOK, d), 0), iota((TOK, d), 1)
    for j in range(TOK // d):
        part = jnp.where(lanes == tokens - j * d, total, 0.0)
        total_log[:, j * d : (j + 1) * d] = jnp.sum(part, axis=0, keepdims=True)
    fetch.wait()


def finish(copies, weight, *arrays):
    return pl.pallas_call(
        finish_body,
        in_specs=[WHOLE] * len(arrays) + [pl.BlockSpec(memory_space=pl.ANY)],
        out_specs=[WHOLE] * 3,
        out_shape=[VMEM((copies, TOK, HEAD_DIM), BF16), VMEM((1, TOK), F32), VMEM(weight.shape, BF16)],
        scratch_shapes=[pltpu.SemaphoreType.DMA],
        name="finish",
    )(*held(*arrays), pltpu.with_memory_space_constraint(weight, pltpu.HBM))


def mix_body(heads, weight, log, out, total_log):
    rows = jnp.concatenate([heads[j] for j in range(heads.shape[0])], axis=1)
    out[...] = jnp.dot(rows, weight[...], preferred_element_type=F32).astype(BF16)
    total_log[...] = log[...]


def mix(heads, weight, log):
    return pl.pallas_call(
        mix_body,
        in_specs=[WHOLE] * 3,
        out_specs=[WHOLE] * 2,
        out_shape=[jax.ShapeDtypeStruct((TOK, weight.shape[1]), BF16), jax.ShapeDtypeStruct(log.shape, F32)],
        name="mix",
    )(*held(heads, weight, log))


def swap(blocks, axis):
    return lax.all_to_all(blocks, axis, split_axis=0, concat_axis=0, tiled=True)


SP = ("z", "yc")


def behind(block, distance):
    count = lax.axis_size(SP)
    return lax.ppermute(block, SP, [(i - distance, i) for i in range(distance, count)])


def other_core(block):
    return lax.ppermute(block, SP, [(i, i ^ 1) for i in range(lax.axis_size(SP))])


def round_the_back(block):
    count = lax.axis_size(SP)

    def chip(z, y, core):
        return z * PLANE + (y % 8) * 2 + core

    places = [(z, y, core) for z in range(count // PLANE) for y in range(8) for core in range(2)]
    block = lax.ppermute(block, SP, [(chip(z, y, core), chip(z, y - 2, core)) for z, y, core in places])
    second = [(chip(z, y - 2, core), chip(z, y, core) + REACH) for z, y, core in places]
    return lax.ppermute(block, SP, [(a, b) for a, b in second if b < count])


def local(tokens, query_weight, key_weight, value_weight, out_weight):
    even = lax.axis_index("yc") % 2 == 0
    queries, near, far, pack = project(tokens, query_weight, key_weight, value_weight)
    four = behind(far, 4)
    eight = round_the_back(far)
    two = behind(pack, 2)
    six = behind(four, 2)
    sent = (jnp.where(even, pack, two), jnp.where(even, two[: 2 * TOK], four))
    odd_near = other_core(jnp.concatenate(sent, axis=0))
    partial = first(queries, near, pack, odd_near, two, four)
    odd_near, six, eight = lax.optimization_barrier((odd_near, six, eight))
    sent = (jnp.where(even, four, six), jnp.where(even, six, eight))
    odd_far = other_core(jnp.concatenate(sent, axis=0))
    merged, total_log, mix_weight = finish(
        lax.axis_size("tp"), out_weight, queries, odd_far, six, eight, *partial
    )
    heads = swap(merged, "tp")
    return mix(heads, mix_weight, total_log)


def solution(mesh):
    devices = mesh.devices
    planes = Mesh(devices.reshape(devices.shape[0] // PLANE, PLANE, devices.shape[1]), ("z", "yc", "tp"))
    sp = ("z", "yc")
    return jax.shard_map(
        local,
        mesh=planes,
        in_specs=(P(sp, None), P(None, "tp"), P(None, "tp"), P(None, "tp"), P(None, "tp")),
        out_specs=(P(sp, "tp"), P("tp", sp)),
        check_vma=False,
    )
```

```python
import jax
import jax.numpy as jnp
from jax import lax
from jax.experimental import pallas as pl
from jax.experimental.pallas import tpu as pltpu
from jax.sharding import Mesh
from jax.sharding import PartitionSpec as P

HEAD_DIM = 128
TOK = 256
PLANE = 16
BAND = 128
MIDDLE_DILATION = 4
FAR_DILATION = 16
REACH = 8
SCALE = HEAD_DIM**-0.5
PIECES = 2
F32 = jnp.float32
BF16 = jnp.bfloat16
VMEM = pltpu.VMEM
WHOLE = pl.BlockSpec(memory_space=pltpu.VMEM)


def held(*arrays):
    return [pltpu.with_memory_space_constraint(a, pltpu.VMEM) for a in arrays]


def iota(shape, dim):
    return lax.broadcasted_iota(jnp.int32, shape, dim)


def head_slope():
    head = lax.axis_index("tp")
    return jnp.where(head == 0, 2.0, jnp.where(head == 1, 0.5, jnp.where(head == 2, 0.125, 0.03125)))


def times_transposed(a, b):
    return lax.dot_general(a, b, (((1,), (1,)), ((), ())), preferred_element_type=F32)


def soft(scores, valid, values):
    scores = jnp.where(valid, scores, -jnp.inf)
    highest = jnp.max(scores, axis=1, keepdims=True)
    weights = jnp.exp(scores - highest)
    total = jnp.sum(weights, axis=1, keepdims=True)
    probs = (weights * (1.0 / total)).astype(BF16)
    return jnp.dot(probs, values, preferred_element_type=F32), highest + jnp.log(total)


def banded(queries, keys, values, slope, has_prior):
    shape = (TOK, TOK + BAND)
    spacing = iota(shape, 0) + BAND - iota(shape, 1)
    first = jnp.where(has_prior, 0, BAND)
    valid = (spacing >= 0) & (spacing <= BAND) & (iota(shape, 1) >= first)
    scores = times_transposed(queries, keys) * SCALE - slope * spacing.astype(F32)
    return soft(scores, valid, values)


def project_body(tok_hbm, wq_hbm, wk_hbm, wv_hbm, queries, near, far, pack, tok, wq, wk, wv, sems):
    d = HEAD_DIM
    piece = tok.shape[1] // PIECES
    spans = [pl.ds(i * piece, piece) for i in range(PIECES)]
    tokens_in = [pltpu.make_async_copy(tok_hbm.at[:, span], tok.at[:, span], sems.at[3, i]) for i, span in enumerate(spans)]
    weights_in = [
        [pltpu.make_async_copy(source.at[span], target.at[span], sems.at[j, i]) for i, span in enumerate(spans)]
        for j, (source, target) in enumerate(((wk_hbm, wk), (wv_hbm, wv), (wq_hbm, wq)))
    ]
    for i in range(PIECES):
        tokens_in[i].start()
        weights_in[0][i].start()
    for part in weights_in[1] + weights_in[2]:
        part.start()
    for j, weight in enumerate((wk, wv, wq)):
        total = None
        for i in range(PIECES):
            if j == 0:
                tokens_in[i].wait()
            weights_in[j][i].wait()
            part = slice(i * piece, (i + 1) * piece)
            product = jnp.dot(tok[:, part], weight[part], preferred_element_type=F32)
            total = product if total is None else total + product
        rows = total.astype(BF16)
        if j == 2:
            for group in range(3):
                queries[group] = rows[:, group * d : (group + 1) * d]
            break
        far[j * TOK : (j + 1) * TOK] = rows[:, 2 * d :]
        pack[j * TOK : (j + 1) * TOK] = rows[:, 2 * d :]
        pack[(2 + j) * TOK : (3 + j) * TOK] = rows[:, d : 2 * d]
        near[j] = rows[:BAND, :d]
        pack[4 * TOK + j * BAND : 4 * TOK + (j + 1) * BAND] = rows[BAND:, :d]


def project(tokens, wq, wk, wv):
    d = HEAD_DIM
    return pl.pallas_call(
        project_body,
        in_specs=[pl.BlockSpec(memory_space=pl.ANY)] * 4,
        out_specs=[WHOLE] * 4,
        out_shape=[
            VMEM((3, TOK, d), BF16),
            VMEM((2, BAND, d), BF16),
            VMEM((2 * TOK, d), BF16),
            VMEM((4 * TOK + 2 * BAND, d), BF16),
        ],
        scratch_shapes=[pltpu.VMEM(a.shape, a.dtype) for a in (tokens, wq, wk, wv)]
        + [pltpu.SemaphoreType.DMA((4, PIECES))],
        name="project",
    )(*[pltpu.with_memory_space_constraint(a, pltpu.HBM) for a in (tokens, wq, wk, wv)])


class Far:
    def __init__(self, queries, slope, place):
        self.queries, self.slope, self.place = queries, slope / (FAR_DILATION * BAND), place
        self.apart = iota((TOK, TOK), 0) - iota((TOK, TOK), 1)
        self.bias = jnp.where(self.apart % FAR_DILATION == 0, self.slope * self.apart.astype(F32), jnp.inf)

    def scores(self, places, keys):
        ahead = jnp.where(self.place >= places, self.slope * (TOK * places), jnp.inf)
        part = times_transposed(self.queries, keys) * SCALE - self.bias - ahead
        if places == 0:
            part = jnp.where(self.apart >= 0, part, -jnp.inf)
        if places == REACH:
            part = jnp.where(self.apart <= 0, part, -jnp.inf)
        return part

    def gather(self, blocks, highest=None):
        scores = [self.scores(places, ref[at : at + TOK]) for places, ref, at in blocks]
        top = scores[0]
        for part in scores[1:]:
            top = jnp.maximum(top, part)
        top = jnp.max(top, axis=1, keepdims=True)
        highest = top if highest is None else jnp.maximum(highest, top)
        total, rows = None, None
        for part, (_, ref, at) in zip(scores, blocks):
            weight = jnp.exp(part - highest)
            piece = jnp.dot(weight.astype(BF16), ref[at + TOK : at + 2 * TOK], preferred_element_type=F32)
            total = weight if total is None else total + weight
            rows = piece if rows is None else rows + piece
        return highest, jnp.sum(total, axis=1, keepdims=True), rows


def place_here():
    return lax.axis_index("z") * PLANE + lax.axis_index("yc")


def first_body(queries, near, own, one, two, four, attended, far_rows, stats):
    slope = head_slope()
    place = place_here()
    b, at = BAND, 4 * TOK
    keys = jnp.concatenate((one[at : at + b], near[0], own[at : at + b]), axis=0)
    values = jnp.concatenate((one[at + b : at + 2 * b], near[1], own[at + b : at + 2 * b]), axis=0)
    first, first_log = banded(queries[0], keys, values, slope / b, place > 0)

    k_at, v_at = slice(2 * TOK, 3 * TOK), slice(3 * TOK, 4 * TOK)
    keys = jnp.concatenate((two[k_at], one[k_at], own[k_at]), axis=0)
    values = jnp.concatenate((two[v_at], one[v_at], own[v_at]), axis=0)
    shape = (TOK, 3 * TOK)
    window = MIDDLE_DILATION * BAND
    spacing = iota(shape, 0) + window - iota(shape, 1)
    begin = jnp.maximum(window - place * TOK, 0)
    valid = (spacing >= 0) & (spacing <= window) & (spacing % MIDDLE_DILATION == 0)
    valid = valid & (iota(shape, 1) >= begin)
    scores = times_transposed(queries[1], keys) * SCALE - (slope / window) * spacing.astype(F32)
    second, second_log = soft(scores, valid, values)

    highest = jnp.maximum(first_log, second_log)
    first_share, second_share = jnp.exp(first_log - highest), jnp.exp(second_log - highest)
    total = first_share + second_share
    inverse = 1.0 / total
    attended[...] = (first_share * inverse) * first + (second_share * inverse) * second
    log = highest + jnp.log(total)

    blocks = ((0, own, 0), (1, one, 0), (2, two, 0), (3, one, 4 * TOK + 2 * BAND), (4, four, 0))
    highest, total, rows = Far(queries[2], slope, place).gather(blocks)
    far_rows[...] = rows
    lanes = iota(stats.shape, 1)
    stats[...] = jnp.where(lanes == 0, log, jnp.where(lanes == 1, highest, total))


def first(*arrays):
    shape = (TOK, HEAD_DIM)
    return pl.pallas_call(
        first_body,
        in_specs=[WHOLE] * len(arrays),
        out_specs=[WHOLE] * 3,
        out_shape=[VMEM(shape, F32)] * 3,
        name="first",
    )(*held(*arrays))


def finish_body(queries, odd, six, eight, attended, far_rows, stats, mix_hbm, merged, total_log, mix_weight, sem):
    d = HEAD_DIM
    fetch = pltpu.make_async_copy(mix_hbm, mix_weight, sem)
    fetch.start()
    blocks = ((5, odd, 0), (6, six, 0), (7, odd, 2 * TOK), (8, eight, 0))
    other_log, before, sum_before = stats[:, 0:1], stats[:, 1:2], stats[:, 2:3]
    highest, total, rows = Far(queries[2], head_slope(), place_here()).gather(blocks, before)
    kept = jnp.exp(before - highest)
    total = total + kept * sum_before
    rows = (rows + kept * far_rows[...]) * (1.0 / total)
    far_log = highest + jnp.log(total)

    highest = jnp.maximum(other_log, far_log)
    total = highest + jnp.log(jnp.exp(other_log - highest) + jnp.exp(far_log - highest))
    both = jnp.exp(other_log - total) * attended[...] + jnp.exp(far_log - total) * rows
    both = both.astype(BF16)
    for j in range(merged.shape[0]):
        merged[j] = both
    tokens, lanes = iota((TOK, d), 0), iota((TOK, d), 1)
    for j in range(TOK // d):
        part = jnp.where(lanes == tokens - j * d, total, 0.0)
        total_log[:, j * d : (j + 1) * d] = jnp.sum(part, axis=0, keepdims=True)
    fetch.wait()


def finish(copies, weight, *arrays):
    return pl.pallas_call(
        finish_body,
        in_specs=[WHOLE] * len(arrays) + [pl.BlockSpec(memory_space=pl.ANY)],
        out_specs=[WHOLE] * 3,
        out_shape=[VMEM((copies, TOK, HEAD_DIM), BF16), VMEM((1, TOK), F32), VMEM(weight.shape, BF16)],
        scratch_shapes=[pltpu.SemaphoreType.DMA],
        name="finish",
    )(*held(*arrays), pltpu.with_memory_space_constraint(weight, pltpu.HBM))


def mix_body(heads, weight, log, out, total_log):
    rows = jnp.concatenate([heads[j] for j in range(heads.shape[0])], axis=1)
    out[...] = jnp.dot(rows, weight[...], preferred_element_type=F32).astype(BF16)
    total_log[...] = log[...]


def mix(heads, weight, log):
    return pl.pallas_call(
        mix_body,
        in_specs=[WHOLE] * 3,
        out_specs=[WHOLE] * 2,
        out_shape=[jax.ShapeDtypeStruct((TOK, weight.shape[1]), BF16), jax.ShapeDtypeStruct(log.shape, F32)],
        name="mix",
    )(*held(heads, weight, log))


def swap(blocks, axis):
    return lax.all_to_all(blocks, axis, split_axis=0, concat_axis=0, tiled=True)


SP = ("z", "yc")


def behind(block, distance):
    count = lax.axis_size(SP)
    return lax.ppermute(block, SP, [(i - distance, i) for i in range(distance, count)])


def other_core(block):
    return lax.ppermute(block, SP, [(i, i ^ 1) for i in range(lax.axis_size(SP))])


def round_the_back(block):
    count = lax.axis_size(SP)

    def chip(z, y, core):
        return z * PLANE + (y % 8) * 2 + core

    places = [(z, y, core) for z in range(count // PLANE) for y in range(8) for core in range(2)]
    block = lax.ppermute(block, SP, [(chip(z, y, core), chip(z, y - 2, core)) for z, y, core in places])
    second = [(chip(z, y - 2, core), chip(z, y, core) + REACH) for z, y, core in places]
    return lax.ppermute(block, SP, [(a, b) for a, b in second if b < count])


def local(tokens, query_weight, key_weight, value_weight, out_weight):
    even = lax.axis_index("yc") % 2 == 0
    queries, near, far, pack = project(tokens, query_weight, key_weight, value_weight)
    four = behind(far, 4)
    eight = round_the_back(far)
    two = behind(pack, 2)
    six = behind(four, 2)
    sent = (jnp.where(even, pack, two), jnp.where(even, two[: 2 * TOK], four))
    odd_near = other_core(jnp.concatenate(sent, axis=0))
    partial = first(queries, near, pack, odd_near, two, four)
    odd_near, six, eight = lax.optimization_barrier((odd_near, six, eight))
    sent = (jnp.where(even, four, six), jnp.where(even, six, eight))
    odd_far = other_core(jnp.concatenate(sent, axis=0))
    merged, total_log, mix_weight = finish(
        lax.axis_size("tp"), out_weight, queries, odd_far, six, eight, *partial
    )
    heads = swap(merged, "tp")
    return mix(heads, mix_weight, total_log)


def solution(mesh):
    devices = mesh.devices
    planes = Mesh(devices.reshape(devices.shape[0] // PLANE, PLANE, devices.shape[1]), ("z", "yc", "tp"))
    sp = ("z", "yc")
    return jax.shard_map(
        local,
        mesh=planes,
        in_specs=(P(sp, None), P(None, "tp"), P(None, "tp"), P(None, "tp"), P(None, "tp")),
        out_specs=(P(sp, "tp"), P("tp", sp)),
        check_vma=False,
    )
```

```python
import jax
import jax.numpy as jnp
from jax import lax
from jax.experimental import pallas as pl
from jax.experimental.pallas import tpu as pltpu
from jax.sharding import Mesh
from jax.sharding import PartitionSpec as P

HEAD_DIM = 128
TOK = 256
PLANE = 16
BAND = 128
MIDDLE_DILATION = 4
FAR_DILATION = 16
REACH = 8
SCALE = HEAD_DIM**-0.5
F32 = jnp.float32
BF16 = jnp.bfloat16
VMEM = pltpu.VMEM
WHOLE = pl.BlockSpec(memory_space=pltpu.VMEM)


def held(*arrays):
    return [pltpu.with_memory_space_constraint(a, pltpu.VMEM) for a in arrays]


def iota(shape, dim):
    return lax.broadcasted_iota(jnp.int32, shape, dim)


def head_slope():
    head = lax.axis_index("tp")
    return jnp.where(head == 0, 2.0, jnp.where(head == 1, 0.5, jnp.where(head == 2, 0.125, 0.03125)))


def times_transposed(a, b):
    return lax.dot_general(a, b, (((1,), (1,)), ((), ())), preferred_element_type=F32)


def soft(scores, valid, values):
    scores = jnp.where(valid, scores, -jnp.inf)
    highest = jnp.max(scores, axis=1, keepdims=True)
    weights = jnp.exp(scores - highest)
    total = jnp.sum(weights, axis=1, keepdims=True)
    probs = (weights * (1.0 / total)).astype(BF16)
    return jnp.dot(probs, values, preferred_element_type=F32), highest + jnp.log(total)


def banded(queries, keys, values, slope, has_prior):
    shape = (TOK, TOK + BAND)
    spacing = iota(shape, 0) + BAND - iota(shape, 1)
    first = jnp.where(has_prior, 0, BAND)
    valid = (spacing >= 0) & (spacing <= BAND) & (iota(shape, 1) >= first)
    scores = times_transposed(queries, keys) * SCALE - slope * spacing.astype(F32)
    return soft(scores, valid, values)


def project_body(tok_hbm, wq_hbm, wk_hbm, wv_hbm, queries, near, far, pack, tok, wq, wk, wv, sems):
    pairs = ((tok_hbm, tok), (wk_hbm, wk), (wv_hbm, wv), (wq_hbm, wq))
    copies = []
    for j, (source, target) in enumerate(pairs):
        half = source.shape[0] // 2
        parts = [
            pltpu.make_async_copy(source.at[pl.ds(i * half, half)], target.at[pl.ds(i * half, half)], sems.at[j, i])
            for i in range(2)
        ]
        for part in parts:
            part.start()
        copies.append(parts)

    def arrive(j):
        for part in copies[j]:
            part.wait()

    d = HEAD_DIM
    arrive(0)
    for j, weight in enumerate((wk, wv)):
        arrive(j + 1)
        rows = jnp.dot(tok[...], weight[...], preferred_element_type=F32).astype(BF16)
        far[j * TOK : (j + 1) * TOK] = rows[:, 2 * d :]
        pack[j * TOK : (j + 1) * TOK] = rows[:, 2 * d :]
        pack[(2 + j) * TOK : (3 + j) * TOK] = rows[:, d : 2 * d]
        near[j] = rows[:BAND, :d]
        pack[4 * TOK + j * BAND : 4 * TOK + (j + 1) * BAND] = rows[BAND:, :d]
    arrive(3)
    rows = jnp.dot(tok[...], wq[...], preferred_element_type=F32).astype(BF16)
    for j in range(3):
        queries[j] = rows[:, j * d : (j + 1) * d]


def project(tokens, wq, wk, wv):
    d = HEAD_DIM
    return pl.pallas_call(
        project_body,
        in_specs=[pl.BlockSpec(memory_space=pl.ANY)] * 4,
        out_specs=[WHOLE] * 4,
        out_shape=[
            VMEM((3, TOK, d), BF16),
            VMEM((2, BAND, d), BF16),
            VMEM((2 * TOK, d), BF16),
            VMEM((4 * TOK + 2 * BAND, d), BF16),
        ],
        scratch_shapes=[pltpu.VMEM(a.shape, a.dtype) for a in (tokens, wq, wk, wv)] + [pltpu.SemaphoreType.DMA((4, 2))],
        name="project",
    )(*[pltpu.with_memory_space_constraint(a, pltpu.HBM) for a in (tokens, wq, wk, wv)])


class Far:
    def __init__(self, queries, slope, place):
        self.queries, self.slope, self.place = queries, slope / (FAR_DILATION * BAND), place
        self.apart = iota((TOK, TOK), 0) - iota((TOK, TOK), 1)
        self.bias = jnp.where(self.apart % FAR_DILATION == 0, self.slope * self.apart.astype(F32), jnp.inf)

    def scores(self, places, keys):
        ahead = jnp.where(self.place >= places, self.slope * (TOK * places), jnp.inf)
        part = times_transposed(self.queries, keys) * SCALE - self.bias - ahead
        if places == 0:
            part = jnp.where(self.apart >= 0, part, -jnp.inf)
        if places == REACH:
            part = jnp.where(self.apart <= 0, part, -jnp.inf)
        return part

    def gather(self, blocks, highest=None):
        scores = [self.scores(places, ref[at : at + TOK]) for places, ref, at in blocks]
        top = scores[0]
        for part in scores[1:]:
            top = jnp.maximum(top, part)
        top = jnp.max(top, axis=1, keepdims=True)
        highest = top if highest is None else jnp.maximum(highest, top)
        total, rows = None, None
        for part, (_, ref, at) in zip(scores, blocks):
            weight = jnp.exp(part - highest)
            piece = jnp.dot(weight.astype(BF16), ref[at + TOK : at + 2 * TOK], preferred_element_type=F32)
            total = weight if total is None else total + weight
            rows = piece if rows is None else rows + piece
        return highest, jnp.sum(total, axis=1, keepdims=True), rows


def place_here():
    return lax.axis_index("z") * PLANE + lax.axis_index("yc")


def early_body(queries, own, two, four, far_rows, stats):
    blocks = ((0, own, 0), (2, two, 0), (4, four, 0))
    highest, total, rows = Far(queries[2], head_slope(), place_here()).gather(blocks)
    far_rows[...] = rows
    stats[...] = jnp.where(iota(stats.shape, 1) == 0, highest, total)


def early(*arrays):
    return pl.pallas_call(
        early_body,
        in_specs=[WHOLE] * len(arrays),
        out_specs=[WHOLE] * 2,
        out_shape=[VMEM((TOK, HEAD_DIM), F32)] * 2,
        name="early",
    )(*held(*arrays))


def first_body(queries, near, own, one, two, early_rows, early_stats, attended, far_rows, stats):
    slope = head_slope()
    place = place_here()
    b, at = BAND, 4 * TOK
    keys = jnp.concatenate((one[at : at + b], near[0], own[at : at + b]), axis=0)
    values = jnp.concatenate((one[at + b : at + 2 * b], near[1], own[at + b : at + 2 * b]), axis=0)
    first, first_log = banded(queries[0], keys, values, slope / b, place > 0)

    k_at, v_at = slice(2 * TOK, 3 * TOK), slice(3 * TOK, 4 * TOK)
    keys = jnp.concatenate((two[k_at], one[k_at], own[k_at]), axis=0)
    values = jnp.concatenate((two[v_at], one[v_at], own[v_at]), axis=0)
    shape = (TOK, 3 * TOK)
    window = MIDDLE_DILATION * BAND
    spacing = iota(shape, 0) + window - iota(shape, 1)
    begin = jnp.maximum(window - place * TOK, 0)
    valid = (spacing >= 0) & (spacing <= window) & (spacing % MIDDLE_DILATION == 0)
    valid = valid & (iota(shape, 1) >= begin)
    scores = times_transposed(queries[1], keys) * SCALE - (slope / window) * spacing.astype(F32)
    second, second_log = soft(scores, valid, values)

    highest = jnp.maximum(first_log, second_log)
    first_share, second_share = jnp.exp(first_log - highest), jnp.exp(second_log - highest)
    total = first_share + second_share
    inverse = 1.0 / total
    attended[...] = (first_share * inverse) * first + (second_share * inverse) * second
    log = highest + jnp.log(total)

    blocks = ((1, one, 0), (3, one, 4 * TOK + 2 * BAND))
    before = early_stats[:, 0:1]
    highest, total, rows = Far(queries[2], slope, place).gather(blocks, before)
    kept = jnp.exp(before - highest)
    total = total + kept * early_stats[:, 1:2]
    far_rows[...] = rows + kept * early_rows[...]
    lanes = iota(stats.shape, 1)
    stats[...] = jnp.where(lanes == 0, log, jnp.where(lanes == 1, highest, total))


def first(*arrays):
    shape = (TOK, HEAD_DIM)
    return pl.pallas_call(
        first_body,
        in_specs=[WHOLE] * len(arrays),
        out_specs=[WHOLE] * 3,
        out_shape=[VMEM(shape, F32)] * 3,
        name="first",
    )(*held(*arrays))


def finish_body(queries, odd, six, eight, attended, far_rows, stats, mix_hbm, merged, total_log, mix_weight, sem):
    d = HEAD_DIM
    fetch = pltpu.make_async_copy(mix_hbm, mix_weight, sem)
    fetch.start()
    blocks = ((5, odd, 0), (6, six, 0), (7, odd, 2 * TOK), (8, eight, 0))
    other_log, before, sum_before = stats[:, 0:1], stats[:, 1:2], stats[:, 2:3]
    highest, total, rows = Far(queries[2], head_slope(), place_here()).gather(blocks, before)
    kept = jnp.exp(before - highest)
    total = total + kept * sum_before
    rows = (rows + kept * far_rows[...]) * (1.0 / total)
    far_log = highest + jnp.log(total)

    highest = jnp.maximum(other_log, far_log)
    total = highest + jnp.log(jnp.exp(other_log - highest) + jnp.exp(far_log - highest))
    both = jnp.exp(other_log - total) * attended[...] + jnp.exp(far_log - total) * rows
    both = both.astype(BF16)
    for j in range(merged.shape[0]):
        merged[j] = both
    tokens, lanes = iota((TOK, d), 0), iota((TOK, d), 1)
    for j in range(TOK // d):
        part = jnp.where(lanes == tokens - j * d, total, 0.0)
        total_log[:, j * d : (j + 1) * d] = jnp.sum(part, axis=0, keepdims=True)
    fetch.wait()


def finish(copies, weight, *arrays):
    return pl.pallas_call(
        finish_body,
        in_specs=[WHOLE] * len(arrays) + [pl.BlockSpec(memory_space=pl.ANY)],
        out_specs=[WHOLE] * 3,
        out_shape=[VMEM((copies, TOK, HEAD_DIM), BF16), VMEM((1, TOK), F32), VMEM(weight.shape, BF16)],
        scratch_shapes=[pltpu.SemaphoreType.DMA],
        name="finish",
    )(*held(*arrays), pltpu.with_memory_space_constraint(weight, pltpu.HBM))


def mix_body(heads, weight, log, out, total_log):
    rows = jnp.concatenate([heads[j] for j in range(heads.shape[0])], axis=1)
    out[...] = jnp.dot(rows, weight[...], preferred_element_type=F32).astype(BF16)
    total_log[...] = log[...]


def mix(heads, weight, log):
    return pl.pallas_call(
        mix_body,
        in_specs=[WHOLE] * 3,
        out_specs=[WHOLE] * 2,
        out_shape=[jax.ShapeDtypeStruct((TOK, weight.shape[1]), BF16), jax.ShapeDtypeStruct(log.shape, F32)],
        name="mix",
    )(*held(heads, weight, log))


def swap(blocks, axis):
    return lax.all_to_all(blocks, axis, split_axis=0, concat_axis=0, tiled=True)


SP = ("z", "yc")


def behind(block, distance):
    count = lax.axis_size(SP)
    return lax.ppermute(block, SP, [(i - distance, i) for i in range(distance, count)])


def other_core(block):
    return lax.ppermute(block, SP, [(i, i ^ 1) for i in range(lax.axis_size(SP))])


def round_the_back(block):
    count = lax.axis_size(SP)

    def chip(z, y, core):
        return z * PLANE + (y % 8) * 2 + core

    places = [(z, y, core) for z in range(count // PLANE) for y in range(8) for core in range(2)]
    block = lax.ppermute(block, SP, [(chip(z, y, core), chip(z, y - 2, core)) for z, y, core in places])
    second = [(chip(z, y - 2, core), chip(z, y, core) + REACH) for z, y, core in places]
    return lax.ppermute(block, SP, [(a, b) for a, b in second if b < count])


def local(tokens, query_weight, key_weight, value_weight, out_weight):
    even = lax.axis_index("yc") % 2 == 0
    queries, near, far, pack = project(tokens, query_weight, key_weight, value_weight)
    four = behind(far, 4)
    eight = round_the_back(far)
    two = behind(pack, 2)
    six = behind(four, 2)
    sent = (jnp.where(even, pack, two), jnp.where(even, two[: 2 * TOK], four))
    odd_near = other_core(jnp.concatenate(sent, axis=0))
    begun = early(queries, pack, two, four)
    partial = first(queries, near, pack, odd_near, two, *begun)
    odd_near, six, eight = lax.optimization_barrier((odd_near, six, eight))
    sent = (jnp.where(even, four, six), jnp.where(even, six, eight))
    odd_far = other_core(jnp.concatenate(sent, axis=0))
    merged, total_log, mix_weight = finish(
        lax.axis_size("tp"), out_weight, queries, odd_far, six, eight, *partial
    )
    heads = swap(merged, "tp")
    return mix(heads, mix_weight, total_log)


def solution(mesh):
    devices = mesh.devices
    planes = Mesh(devices.reshape(devices.shape[0] // PLANE, PLANE, devices.shape[1]), ("z", "yc", "tp"))
    sp = ("z", "yc")
    return jax.shard_map(
        local,
        mesh=planes,
        in_specs=(P(sp, None), P(None, "tp"), P(None, "tp"), P(None, "tp"), P(None, "tp")),
        out_specs=(P(sp, "tp"), P("tp", sp)),
        check_vma=False,
    )
```
